256 devices in a mesh: grp: 2 (over y), ep: 64 (over z, x), tp: 2 (over core).
Axes of the slice: x: 4, y: 2, z: 16, core: 2. Of those that a mesh axis runs over, the one named last changes fastest.
The devices are a block of a 4x16x16 slice.
Arguments:
- hidden_state: bfloat16 [8192, 1024], P(('grp', 'ep'), 'tp'), parts along dimension 0, may hold values from -6 to 6
- expert_ids: int32 [8192, 4], P(('grp', 'ep')), parts along dimension 0, may hold values from 0 to 63, all different within a row; in each aligned block of 64 rows (0 to 63, 64 to 127, ...) at most 8 rows name the same one
- route_weight: float32 [8192, 4], P(('grp', 'ep')), parts along dimension 0, may hold values from 0.1 to 1
- gate_matrix: bfloat16 [64, 1024, 2048], P('ep', None, 'tp'), may hold values from -0.1875 to 0.1875
- up_matrix: bfloat16 [64, 1024, 2048], P('ep', None, 'tp'), may hold values from -0.1875 to 0.1875
- down_matrix: bfloat16 [64, 2048, 1024], P('ep', 'tp'), may hold values from -2 to 2
- norm_gain: float32 [1024], P('tp'), may hold values from 0.1 to 1.9
Outputs:
- normed_out: bfloat16 [8192, 1024], P(('grp', 'ep'), 'tp'), parts along dimension 0
The draws below stay inside these ranges and needn't reach their ends.
There are 2 independent parts, one for each index of `grp`. The reference program is written for one: setup_inputs(seed, part) draws one part's arguments, and reference() takes and returns one part's arrays. A program takes and returns all parts, laid end to end along the dimension named above; an argument that names none is the same for every part. Nothing has to cross between parts.
Inputs may be any that keep to these rules, and one draw needn't show every extreme that they name: `expert_ids`: each row names 4 different experts. Within the rows of one index of ep (aligned blocks of 64 rows) no expert is named by more than 8 rows, and in some blocks one expert is named by exactly 8 rows. Every expert is named by some row.
All inputs are finite; a program needn't handle non-finite values.
Results may differ from the reference program's by a relative error of at most 0.0065.
Values may be sent and summed in bfloat16 or wider, within the bound.
A program may use at most 64 MiB of HBM per device.

```python
import math
import jax
import jax.numpy as jnp
import numpy as np
from jax import lax

D = 1024
FF = 2048
TOPK = 4
TOK_DEV = 64
EXPERTS = 64
TOKENS = 4096
CAP = 8
N_EP = 64
N_TP = 2


def draw_down_matrix(key, part):
    noise_key = jax.random.fold_in(key, 11)
    scale_key = jax.random.fold_in(key, 23)
    column = jnp.arange(D, dtype=jnp.float32) / D
    jitter = jax.random.uniform(scale_key, (D,), jnp.float32, -0.35, 0.35)
    base = jnp.clip(jax.random.normal(noise_key, (EXPERTS, FF, D), jnp.float32), -6.0, 6.0)
    column_scale = jnp.exp(math.log(10.0) * column + jitter)
    values = base * column_scale[None, None, :] * FF ** (-0.5)
    return jnp.clip(values, -2.0, 2.0).astype(jnp.bfloat16)


def block_scale(key, shape, cuts, low, top_value):
    factor_of = 1.0
    for axis_at, shards_of in cuts:
        heights = jax.random.uniform(jax.random.fold_in(jax.random.fold_in(key, 6), axis_at), (shards_of,), jnp.float32, low / len(cuts), top_value / len(cuts))
        factor_of = factor_of * jnp.repeat(jnp.exp(heights), shape[axis_at] // shards_of).reshape((-1,) + (1,) * (len(shape) - 1 - axis_at))
    return factor_of


def deal_out(key, own, number, rows, number_of, top, bound, slope):
    sequence = jax.random.permutation(key, number_of)
    packed, ordinary = load_shares(number_of, rows * top, bound, slope, True), load_shares(number_of, rows * top, bound, slope, False)
    places = jnp.arange(number_of)

    def named(sizes, offset_by):
        used = int((sizes > 0).sum())
        fixed = max(1, used // 4)
        moved = fixed + (places - fixed + offset_by * (used - fixed)) % max(1, number_of - fixed)
        return jnp.zeros((number_of,), jnp.int32).at[sequence[jnp.where(places < fixed, places, moved)]].set(jnp.asarray(sizes, jnp.int32))

    sizes = jnp.where(number % 4 == 0, named(packed, number // 4), named(ordinary, number - number // 4 - 1))
    mixed = jax.random.permutation(jax.random.fold_in(own, 3), number_of)
    donor, taker = mixed[0:number_of // 2 * 2:2], mixed[1:number_of // 2 * 2:2]
    room = jnp.minimum(sizes[donor] - 1, bound - sizes[taker]) // 2
    room = jnp.where((donor == sequence[0]) | (taker == sequence[0]) | (sizes[taker] == 0), 0, jnp.maximum(room, 0))
    moved = jax.random.randint(jax.random.fold_in(own, 4), (number_of // 2,), 0, 1 << 20) % (room + 1)
    sizes = sizes.at[donor].add(-moved).at[taker].add(moved)
    members = jnp.searchsorted(jnp.cumsum(sizes), jnp.arange(rows * top), side="right").astype(jnp.int32)
    grid = members.reshape(top, rows).T
    grid = grid[jax.random.permutation(jax.random.fold_in(own, 1), rows)]
    offset_by = jax.random.randint(jax.random.fold_in(own, 2), (rows, 1), 0, top)
    return jnp.take_along_axis(grid, (jnp.arange(top)[None, :] + offset_by) % top, axis=1)


def load_shares(number_of, total, reach, slope, full):
    weights = [(1 << 20) // math.isqrt(standing ** slope) + 1 for standing in range(1, number_of + 1)]
    largest = reach if full else min(reach, max(-(-total // number_of), total * weights[0] // sum(weights)))
    least = 1 if total - largest >= number_of - 1 else 0
    counts, rest = [largest] + [least] * (number_of - 1), total - largest - least * (number_of - 1)
    while rest > 0:
        candidates = [i for i in range(1, number_of) if counts[i] < largest] or [i for i in range(1, number_of) if counts[i] < reach]
        whole, budget = sum([weights[i] for i in candidates]), rest
        for i in candidates:
            extra = min(reach - counts[i], max(1, budget * weights[i] // whole), rest)
            counts[i] = counts[i] + extra
            rest = rest - extra
    return np.array(counts)


def centred(rng, extent, width, bound, pieces=(), kind=jnp.bfloat16):
    array = jax.random.normal(rng, extent, jnp.float32) * width
    if len(pieces) > 0:
        array = block_scale(rng, extent, pieces, -0.22, 0.18) * array
    return jnp.clip(array, min=-bound, max=bound).astype(kind)


def setup_inputs(seed: int = 0, part: int = 0) -> dict:
    seeds = jax.random.split(jax.random.key(seed), 8)
    own_keys = jax.random.split(jax.random.fold_in(seeds[7], part), 8)
    hidden_state = centred(own_keys[0], (TOKENS, D), 1.0, 6.0, ((0, 64), (1, 2)))
    expert_ids_keys = jax.random.split(jax.random.fold_in(own_keys[1], 1), TOKENS // TOK_DEV)
    expert_ids_turns = jax.random.permutation(jax.random.fold_in(own_keys[1], 3), TOKENS // TOK_DEV)
    expert_ids = jax.vmap(lambda own, number: deal_out(jax.random.fold_in(own_keys[1], 2), own, number, TOK_DEV, EXPERTS, TOPK, CAP, 2))(expert_ids_keys, expert_ids_turns).reshape((TOKENS, TOPK))
    route_weight = jnp.clip(jnp.exp(math.log(1.0) - 2.3025851 * jax.random.uniform(own_keys[2], (TOKENS, TOPK), jnp.float32) ** block_scale(own_keys[2], (TOKENS, TOPK), ((0, 64),), -0.2, 0.2)), 0.1, 1.0)
    gate_matrix = centred(seeds[3], (EXPERTS, D, FF), D ** -0.5, 0.1875, ((0, 64), (2, 2)))
    up_matrix = centred(seeds[4], (EXPERTS, D, FF), D ** -0.5, 0.1875, ((0, 64), (2, 2)))
    down_matrix = draw_down_matrix(jax.random.fold_in(seeds[7], 71), part)
    norm_gain = jnp.clip(1.0 + 0.18 * jax.random.normal(seeds[6], (D,), jnp.float32), 0.1, 1.9)
    return {"hidden_state": hidden_state, "expert_ids": expert_ids, "route_weight": route_weight, "gate_matrix": gate_matrix, "up_matrix": up_matrix, "down_matrix": down_matrix, "norm_gain": norm_gain}


def slot_ranks(expert_ids):
    blocks = expert_ids.reshape(N_EP, TOK_DEV * TOPK)
    onehot = (blocks[:, :, None] == jnp.arange(EXPERTS, dtype=jnp.int32)[None, None, :]).astype(jnp.int32)
    earlier = jnp.cumsum(onehot, axis=1) - onehot
    return lax.optimization_barrier(jnp.sum(earlier * onehot, axis=2)).astype(jnp.int32).reshape(TOKENS, TOPK)

def reference(hidden_state, expert_ids, route_weight, gate_matrix, up_matrix, down_matrix, norm_gain):
    slot_rank = slot_ranks(expert_ids)
    block_index = (jnp.arange(TOKENS, dtype=jnp.int32) // TOK_DEV)[:, None]
    slot_index = (block_index * CAP + slot_rank).astype(jnp.int32)
    token_ids = jnp.broadcast_to(jnp.arange(TOKENS, dtype=jnp.int32)[:, None], (TOKENS, TOPK))
    slot_table = jnp.zeros((EXPERTS, N_EP * CAP), jnp.int32).at[expert_ids, slot_index].set(token_ids)
    half_width = FF // N_TP

    def one_expert(operands):
        row_index, gate_block, up_block, down_block = operands
        token_rows = hidden_state[row_index]
        gate_pre = jnp.dot(token_rows, gate_block, preferred_element_type=jnp.float32)
        up_pre = jnp.dot(token_rows, up_block, preferred_element_type=jnp.float32)
        activated = (jax.nn.silu(gate_pre) * up_pre).astype(jnp.bfloat16)
        summed_rows = jnp.zeros((token_rows.shape[0], D), jnp.float32)
        for segment in range(N_TP):
            partial_value = jnp.dot(activated[:, segment * half_width:(segment + 1) * half_width], down_block[segment * half_width:(segment + 1) * half_width], preferred_element_type=jnp.float32).astype(jnp.bfloat16)
            partial_value = lax.optimization_barrier(partial_value)
            summed_rows = summed_rows + partial_value.astype(jnp.float32)
        return summed_rows.astype(jnp.bfloat16)
    outputs = lax.map(one_expert, (slot_table, gate_matrix, up_matrix, down_matrix))
    picked = outputs[expert_ids, slot_index]
    combined = lax.optimization_barrier(jnp.sum(route_weight[:, :, None].astype(jnp.float32) * picked.astype(jnp.float32), axis=1))
    mean_square = lax.optimization_barrier(jnp.mean(combined * combined, axis=1, keepdims=True))
    return (combined * lax.rsqrt(mean_square + 1e-05) * norm_gain).astype(jnp.bfloat16)
```

```python
import functools

import jax
import jax.numpy as jnp
from jax import lax
from jax.experimental import pallas as pl
from jax.experimental.pallas import tpu as pltpu
from jax.sharding import PartitionSpec as P

MESH = pl.DeviceIdType.MESH
norm_eps = 1e-05
COLUMNS = 4
STRIDE = 4
SLOTS = COLUMNS * STRIDE
SELF = SLOTS - 1
SOURCE = (0, -STRIDE, STRIDE, 2 * STRIDE)
LANES = 128


def window(slot):
    number = (slot + 5) % SLOTS
    row, column = number // COLUMNS, number % COLUMNS
    return row - 1 - column % 2, column


def kernel(
    planes,
    h_ref, meta_ref, gain_ref, gate_ref, up_ref, down_ref,
    out_ref,
    gate_w, up_w, down_w, blocks, metas, outgoing, mine, other, act, part_out, part_in, own_part,
    answers, returned, weight_hi, weight_lo, near_sum, travel, chain_in, final_in, square_out, square_in,
    w_sem, m_send, m_recv, h_send, h_recv, d_send, d_recv, x_send, x_recv, s_send, s_recv, r_send, r_recv,
    c_send, c_recv, f_send, f_recv, q_send, q_recv,
):
    tokens, width = h_ref.shape
    capacity = outgoing.shape[2]
    rows = SLOTS * capacity
    half = tokens // 2
    top = meta_ref.shape[0] // 2
    core = lax.axis_index("tp")
    me = lax.axis_index("ep")
    plane, column = me // COLUMNS, lax.rem(me, COLUMNS)

    def at(planes_on, columns_on):
        return lax.rem(plane + planes_on + planes, planes) * COLUMNS + lax.rem(
            column + columns_on + COLUMNS, COLUMNS
        )

    def remote(src, dst, send, recv, where):
        return pltpu.make_async_remote_copy(
            src_ref=src, dst_ref=dst, send_sem=send, recv_sem=recv, device_id=where, device_id_type=MESH
        )

    partner = {"tp": 1 - core}

    loads = []
    for side in range(2):
        at_core = (core + side) % 2
        span = pl.ds(pl.multiple_of(at_core * width, width), width)
        for order, (source, target) in enumerate(
            (
                (gate_ref.at[0, span, :], gate_w.at[pl.ds(side * width, width), :]),
                (up_ref.at[0, span, :], up_w.at[pl.ds(side * width, width), :]),
                (down_ref.at[0, :, span], down_w.at[side]),
            )
        ):
            load = pltpu.make_async_copy(source, target, w_sem.at[side * 3 + order])
            load.start()
            loads.append(load)

    greeted = {(STRIDE, 0), (-STRIDE, 0)}
    for slot in range(SLOTS - 1):
        planes_on, columns_on = window(slot)
        greeted.add((planes_on, columns_on))
        greeted.add((-planes_on, (-columns_on) % COLUMNS))
    barrier = pltpu.get_barrier_semaphore()
    for planes_on, columns_on in sorted(greeted):
        pl.semaphore_signal(barrier, inc=1, device_id={"ep": at(planes_on, columns_on)}, device_id_type=MESH)
    pl.semaphore_signal(barrier, inc=1, device_id=partner, device_id_type=MESH)

    row_at = lax.broadcasted_iota(jnp.int32, (rows, LANES), 0)
    number = lax.rem(row_at // capacity + 5, SLOTS)
    row_column = lax.rem(number, COLUMNS)
    row_plane = lax.rem(plane + number // COLUMNS - 1 - lax.rem(row_column, 2) + planes, planes)
    row_expert = (row_plane * COLUMNS + lax.rem(column + row_column, COLUMNS)).astype(jnp.float32)
    row_slot = lax.rem(row_at, capacity).astype(jnp.float32)
    before = (
        lax.broadcasted_iota(jnp.int32, (LANES, LANES), 0) < lax.broadcasted_iota(jnp.int32, (LANES, LANES), 1)
    ).astype(jnp.bfloat16)

    def place(b):
        meta = meta_ref if b == 0 else metas.at[b - 1]
        named = jnp.zeros((rows, LANES), jnp.float32)
        weight = jnp.zeros((rows, LANES), jnp.float32)
        for k in range(top):
            match = meta[k : k + 1, :] == row_expert
            named = named + jnp.where(match, 1.0, 0.0)
            weight = weight + jnp.where(match, meta[top + k : top + k + 1, :], 0.0)
        rank = jnp.dot(named.astype(jnp.bfloat16), before, preferred_element_type=jnp.float32)
        placed = jnp.where(rank == row_slot, named, 0.0)
        block = h_ref[...] if b == 0 else blocks[b - 1]
        chosen = jnp.dot(placed[:, :tokens].astype(jnp.bfloat16), block, preferred_element_type=jnp.float32)
        outgoing[b] = chosen.reshape(SLOTS, capacity, width).astype(jnp.bfloat16)
        weights = (placed * weight).T[:tokens]
        high = weights.astype(jnp.bfloat16)
        weight_hi[b] = high
        weight_lo[b] = (weights - high.astype(jnp.float32)).astype(jnp.bfloat16)

    def send_slots(b, source, target, send, recv, sign):
        for slot in range(SLOTS - 1):
            planes_on, columns_on = window(slot)
            remote(
                source.at[b, slot],
                target.at[b, slot],
                send.at[b],
                recv.at[b],
                {"ep": at(sign * planes_on, sign * columns_on)},
            ).start()
        target[b, SELF] = source[b, SELF]

    def wait_slots(b, buffer, sem):
        span = buffer.at[b, pl.ds(0, SLOTS - 1)]
        pltpu.make_async_copy(span, span, sem.at[b]).wait()

    place(0)
    pl.semaphore_wait(barrier, len(greeted) + 1)

    up_ring, down_ring = {"ep": at(STRIDE, 0)}, {"ep": at(-STRIDE, 0)}
    spans = (pl.ds(0, half), pl.ds(half, half))
    first = []

    def go(copy):
        copy.start()
        first.append(copy)
        return copy

    def block_to(b, source, where, part):
        return go(
            remote(
                source.at[spans[part]],
                blocks.at[b - 1, spans[part]],
                h_send.at[b - 1, part],
                h_recv.at[b - 1, part],
                where,
            )
        )

    meta_up = go(remote(meta_ref, metas.at[0], m_send.at[0], m_recv.at[0], up_ring))
    meta_down = go(remote(meta_ref, metas.at[1], m_send.at[1], m_recv.at[1], down_ring))
    up_low = block_to(1, h_ref, up_ring, 0)
    down_high = block_to(2, h_ref, down_ring, 1)
    up_high = block_to(1, h_ref, up_ring, 1)
    down_low = block_to(2, h_ref, down_ring, 0)
    send_slots(0, outgoing, mine, d_send, d_recv, 1)

    meta_up.wait_recv()
    meta_far = go(remote(metas.at[0], metas.at[2], m_send.at[2], m_recv.at[2], up_ring))
    up_low.wait_recv()
    far_low = block_to(3, blocks.at[0], up_ring, 0)
    down_high.wait_recv()
    far_high = block_to(3, blocks.at[1], down_ring, 1)
    up_high.wait_recv()
    place(1)
    send_slots(1, outgoing, mine, d_send, d_recv, 1)
    meta_down.wait_recv()
    down_low.wait_recv()
    place(2)
    send_slots(2, outgoing, mine, d_send, d_recv, 1)

    def exchange(group):
        for b in group:
            wait_slots(b, mine, d_recv)
        span = pl.ds(group[0], len(group))
        copy = remote(mine.at[span], other.at[span], x_send.at[group[0]], x_recv.at[group[0]], partner)
        return go(copy)

    def experts(group, swap):
        count = len(group) * rows
        span = pl.ds(group[0], len(group))
        swap.wait_recv()
        tokens_in = jnp.concatenate(
            [mine[span].reshape(count, width), other[span].reshape(count, width)], axis=1
        )
        step = 256
        for start in range(0, gate_w.shape[1], step):
            gate = jnp.dot(tokens_in, gate_w[:, start : start + step], preferred_element_type=jnp.float32)
            up = jnp.dot(tokens_in, up_w[:, start : start + step], preferred_element_type=jnp.float32)
            value = gate * (1.0 / (1.0 + jnp.exp(-gate))) * up
            act[pl.ds(0, count), start : start + step] = value.astype(jnp.bfloat16)
        active = act[pl.ds(0, count), :]
        away = jnp.dot(active, down_w[1], preferred_element_type=jnp.float32)
        part_out[span] = away.astype(jnp.bfloat16).reshape(len(group), rows, width)
        copy = go(remote(part_out.at[span], part_in.at[span], s_send.at[group[0]], s_recv.at[group[0]], partner))
        here = jnp.dot(active, down_w[0], preferred_element_type=jnp.float32)
        own_part[span] = here.astype(jnp.bfloat16).reshape(len(group), rows, width)
        return copy

    def answer(group, copy):
        copy.wait_recv()
        for b in group:
            both = own_part[b].astype(jnp.float32) + part_in[b].astype(jnp.float32)
            answers[b] = both.reshape(SLOTS, capacity, width).astype(jnp.bfloat16)
            send_slots(b, answers, returned, r_send, r_recv, -1)

    def combine(b):
        wait_slots(b, returned, r_recv)
        slots = returned[b].reshape(rows, width)
        return jnp.dot(weight_hi[b], slots, preferred_element_type=jnp.float32) + jnp.dot(
            weight_lo[b], slots, preferred_element_type=jnp.float32
        )

    swap = exchange((0,))
    for load in loads:
        load.wait()
    part = experts((0,), swap)

    far_low.wait_recv()
    far_high.wait_recv()
    meta_far.wait_recv()
    place(3)
    send_slots(3, outgoing, mine, d_send, d_recv, 1)

    answer((0,), part)
    swap = exchange((1, 2))
    part = experts((1, 2), swap)
    swap = exchange((3,))
    answer((1, 2), part)
    part = experts((3,), swap)
    answer((3,), part)

    near_sum[0] = combine(0)
    near = combine(1)
    near_sum[1] = near
    travel[0] = near.astype(jnp.bfloat16)
    finals = {}

    def final_to(b, where, part):
        finals[b, part] = go(
            remote(
                travel.at[b - 1, spans[part]],
                final_in.at[b - 1, spans[part]],
                f_send.at[b - 1, part],
                f_recv.at[b - 1, part],
                where,
            )
        )

    final_to(1, down_ring, 1)
    near = combine(2)
    near_sum[2] = near
    travel[1] = near.astype(jnp.bfloat16)
    final_to(2, up_ring, 0)
    travel[2] = combine(3).astype(jnp.bfloat16)
    chains = []
    for part_at, where in ((0, down_ring), (1, up_ring)):
        chains.append(
            go(
                remote(
                    travel.at[2, spans[part_at]],
                    chain_in.at[spans[part_at]],
                    c_send.at[part_at],
                    c_recv.at[part_at],
                    where,
                )
            )
        )
    for part_at, (b, where) in enumerate(((1, down_ring), (2, up_ring))):
        chains[part_at].wait_recv()
        total = near_sum[b, spans[part_at]] + chain_in[spans[part_at]].astype(jnp.float32)
        travel[b - 1, spans[part_at]] = total.astype(jnp.bfloat16)
        final_to(b, where, part_at)
    for copy in finals.values():
        copy.wait_recv()
    combined = near_sum[0] + final_in[0].astype(jnp.float32) + final_in[1].astype(jnp.float32)
    squares = jnp.sum(combined * combined, axis=1, keepdims=True)
    square_out[...] = jnp.broadcast_to(squares, square_out.shape)
    copy = go(remote(square_out, square_in, q_send.at[0], q_recv.at[0], partner))
    copy.wait_recv()
    mean = (squares + square_in[:, :1]) / (2 * width)
    out_ref[...] = (combined * lax.rsqrt(mean + norm_eps) * gain_ref[...]).astype(jnp.bfloat16)

    for copy in first:
        copy.wait_send()
    for b in range(len(SOURCE)):
        wait_slots(b, outgoing, d_send)
        wait_slots(b, answers, r_send)


def solution(mesh):
    experts = mesh.shape["ep"]
    planes = experts // COLUMNS
    assert planes == STRIDE * len(SOURCE) and mesh.shape["tp"] == 2

    def shards(hidden_state, expert_ids, route_weight, gate_matrix, up_matrix, down_matrix, norm_gain):
        tokens, top = expert_ids.shape
        width = hidden_state.shape[1]
        hidden = gate_matrix.shape[2]
        capacity = max(2, 2 * tokens * top // experts)
        rows = SLOTS * capacity
        count = len(SOURCE)
        spare = ((0, 0), (0, LANES - tokens))
        meta = jnp.concatenate(
            [
                jnp.pad(expert_ids.T.astype(jnp.float32), spare, constant_values=-1.0),
                jnp.pad(route_weight.T, spare),
            ]
        )
        vmem, anywhere = pl.BlockSpec(memory_space=pltpu.VMEM), pl.BlockSpec(memory_space=pl.ANY)
        slots = pltpu.VMEM((count, SLOTS, capacity, width), jnp.bfloat16)
        parts = pltpu.VMEM((count, rows, width), jnp.bfloat16)
        dma = pltpu.SemaphoreType.DMA
        return pl.pallas_call(
            functools.partial(kernel, planes),
            out_shape=jax.ShapeDtypeStruct((tokens, width), jnp.bfloat16),
            in_specs=[vmem, vmem, vmem, anywhere, anywhere, anywhere],
            out_specs=vmem,
            scratch_shapes=[
                pltpu.VMEM((2 * width, hidden), jnp.bfloat16),
                pltpu.VMEM((2 * width, hidden), jnp.bfloat16),
                pltpu.VMEM((2, hidden, width), jnp.bfloat16),
                pltpu.VMEM((count - 1, tokens, width), jnp.bfloat16),
                pltpu.VMEM((count - 1, 2 * top, LANES), jnp.float32),
                slots,
                slots,
                slots,
                pltpu.VMEM((2 * rows, hidden), jnp.bfloat16),
                parts,
                parts,
                parts,
                slots,
                slots,
                pltpu.VMEM((count, tokens, rows), jnp.bfloat16),
                pltpu.VMEM((count, tokens, rows), jnp.bfloat16),
                pltpu.VMEM((3, tokens, width), jnp.float32),
                pltpu.VMEM((3, tokens, width), jnp.bfloat16),
                pltpu.VMEM((tokens, width), jnp.bfloat16),
                pltpu.VMEM((2, tokens, width), jnp.bfloat16),
                pltpu.VMEM((tokens, LANES), jnp.float32),
                pltpu.VMEM((tokens, LANES), jnp.float32),
                dma((6,)),
                dma((3,)), dma((3,)),
                dma((3, 2)), dma((3, 2)),
                dma((count,)), dma((count,)),
                dma((count,)), dma((count,)),
                dma((count,)), dma((count,)),
                dma((count,)), dma((count,)),
                dma((2,)), dma((2,)),
                dma((2, 2)), dma((2, 2)),
                dma((1,)), dma((1,)),
            ],
            compiler_params=pltpu.CompilerParams(
                collective_id=0, has_side_effects=True, vmem_limit_bytes=48 * 1024 * 1024
            ),
        )(hidden_state, meta, norm_gain.reshape(1, width), gate_matrix, up_matrix, down_matrix)

    placed = (
        P(("grp", "ep"), "tp"),
        P(("grp", "ep"), None),
        P(("grp", "ep"), None),
        P("ep", None, "tp"),
        P("ep", None, "tp"),
        P("ep", "tp", None),
        P("tp"),
    )
    return jax.shard_map(
        shards, mesh=mesh, in_specs=placed, out_specs=P(("grp", "ep"), "tp"), check_vma=False
    )
```

```python
import functools

import jax
import jax.numpy as jnp
from jax import lax
from jax.experimental import pallas as pl
from jax.experimental.pallas import tpu as pltpu
from jax.sharding import PartitionSpec as P

MESH = pl.DeviceIdType.MESH
norm_eps = 1e-05
COLUMNS = 4
STRIDE = 4
SLOTS = COLUMNS * STRIDE
SELF = SLOTS - 1
SOURCE = (0, -STRIDE, STRIDE, 2 * STRIDE)
LANES = 128
CHUNKS = 2


def window(slot):
    number = (slot + 5) % SLOTS
    row, column = number // COLUMNS, number % COLUMNS
    return row - 1 - column % 2, column


def kernel(
    planes,
    h_hbm, ids_hbm, route_hbm, gain_hbm, gate_ref, up_ref, down_ref,
    out_ref,
    h_ref, ids_ref, route_ref, gain_ref, meta_ref, gate_w, up_w, down_w, blocks, metas, outgoing, mine, other, act, part_out, part_in, own_part,
    answers, returned, weight_hi, weight_lo, near_sum, travel, chain_in, final_in, square_out, square_in,
    i_sem, w_sem, m_send, m_recv, h_send, h_recv, d_send, d_recv, x_send, x_recv, s_send, s_recv, r_send, r_recv,
    c_send, c_recv, f_send, f_recv, q_send, q_recv,
):
    tokens, width = h_ref.shape
    capacity = outgoing.shape[2]
    rows = SLOTS * capacity
    half = tokens // 2
    top = ids_ref.shape[0]
    inputs = []
    for order, (source, target) in enumerate(
        ((ids_hbm, ids_ref), (route_hbm, route_ref), (h_hbm, h_ref), (gain_hbm, gain_ref))
    ):
        load = pltpu.make_async_copy(source, target, i_sem.at[order])
        load.start()
        inputs.append(load)
    core = lax.axis_index("tp")
    me = lax.axis_index("ep")
    plane, column = me // COLUMNS, lax.rem(me, COLUMNS)

    def at(planes_on, columns_on):
        return lax.rem(plane + planes_on + planes, planes) * COLUMNS + lax.rem(
            column + columns_on + COLUMNS, COLUMNS
        )

    def remote(src, dst, send, recv, where):
        return pltpu.make_async_remote_copy(
            src_ref=src, dst_ref=dst, send_sem=send, recv_sem=recv, device_id=where, device_id_type=MESH
        )

    partner = {"tp": 1 - core}

    greeted = {(STRIDE, 0), (-STRIDE, 0)}
    for slot in range(SLOTS - 1):
        planes_on, columns_on = window(slot)
        greeted.add((planes_on, columns_on))
        greeted.add((-planes_on, (-columns_on) % COLUMNS))
    barrier = pltpu.get_barrier_semaphore()
    for planes_on, columns_on in sorted(greeted):
        pl.semaphore_signal(barrier, inc=1, device_id={"ep": at(planes_on, columns_on)}, device_id_type=MESH)
    pl.semaphore_signal(barrier, inc=1, device_id=partner, device_id_type=MESH)

    row_at = lax.broadcasted_iota(jnp.int32, (rows, LANES), 0)
    number = lax.rem(row_at // capacity + 5, SLOTS)
    row_column = lax.rem(number, COLUMNS)
    row_plane = lax.rem(plane + number // COLUMNS - 1 - lax.rem(row_column, 2) + planes, planes)
    row_expert = (row_plane * COLUMNS + lax.rem(column + row_column, COLUMNS)).astype(jnp.float32)
    row_slot = lax.rem(row_at, capacity).astype(jnp.float32)
    before = (
        lax.broadcasted_iota(jnp.int32, (LANES, LANES), 0) < lax.broadcasted_iota(jnp.int32, (LANES, LANES), 1)
    ).astype(jnp.bfloat16)

    def place(b):
        meta = meta_ref if b == 0 else metas.at[b - 1]
        named = jnp.zeros((rows, LANES), jnp.float32)
        weight = jnp.zeros((rows, LANES), jnp.float32)
        for k in range(top):
            match = meta[k : k + 1, :] == row_expert
            named = named + jnp.where(match, 1.0, 0.0)
            weight = weight + jnp.where(match, meta[top + k : top + k + 1, :], 0.0)
        rank = jnp.dot(named.astype(jnp.bfloat16), before, preferred_element_type=jnp.float32)
        placed = jnp.where(rank == row_slot, named, 0.0)
        block = h_ref[...] if b == 0 else blocks[b - 1]
        chosen = jnp.dot(placed[:, :tokens].astype(jnp.bfloat16), block, preferred_element_type=jnp.float32)
        outgoing[b] = chosen.reshape(SLOTS, capacity, width).astype(jnp.bfloat16)
        weights = (placed * weight).T[:tokens]
        high = weights.astype(jnp.bfloat16)
        weight_hi[b] = high
        weight_lo[b] = (weights - high.astype(jnp.float32)).astype(jnp.bfloat16)

    def send_slots(b, source, target, send, recv, sign):
        for slot in range(SLOTS - 1):
            planes_on, columns_on = window(slot)
            remote(
                source.at[b, slot],
                target.at[b, slot],
                send.at[b],
                recv.at[b],
                {"ep": at(sign * planes_on, sign * columns_on)},
            ).start()
        target[b, SELF] = source[b, SELF]

    def wait_slots(b, buffer, sem):
        span = buffer.at[b, pl.ds(0, SLOTS - 1)]
        pltpu.make_async_copy(span, span, sem.at[b]).wait()

    for load in inputs:
        load.wait()
    loads = []
    for side in range(2):
        at_core = (core + side) % 2
        span = pl.ds(pl.multiple_of(at_core * width, width), width)
        for order, (source, target) in enumerate(
            (
                (gate_ref.at[0, span, :], gate_w.at[pl.ds(side * width, width), :]),
                (up_ref.at[0, span, :], up_w.at[pl.ds(side * width, width), :]),
                (down_ref.at[0, :, span], down_w.at[side]),
            )
        ):
            load = pltpu.make_async_copy(source, target, w_sem.at[side * 3 + order])
            load.start()
            loads.append(load)

    meta_ref[...] = jnp.full(meta_ref.shape, -1.0, jnp.float32)
    meta_ref[0:top, 0:tokens] = ids_ref[...].astype(jnp.float32)
    meta_ref[top : 2 * top, 0:tokens] = route_ref[...]
    place(0)
    pl.semaphore_wait(barrier, len(greeted) + 1)

    up_ring, down_ring = {"ep": at(STRIDE, 0)}, {"ep": at(-STRIDE, 0)}
    quarter = half // CHUNKS
    chunks = [pl.ds(part * quarter, quarter) for part in range(2 * CHUNKS)]
    relayed = (range(CHUNKS), range(CHUNKS, 2 * CHUNKS))
    spans = (pl.ds(0, half), pl.ds(half, half))
    first = []

    def go(copy):
        copy.start()
        first.append(copy)
        return copy

    def block_to(b, source, where, rows_in, sem):
        return go(
            remote(
                source.at[rows_in],
                blocks.at[b - 1, rows_in],
                h_send.at[b - 1, sem],
                h_recv.at[b - 1, sem],
                where,
            )
        )

    ways = (up_ring, down_ring)
    meta_near = [
        go(remote(meta_ref, metas.at[way], m_send.at[way], m_recv.at[way], where)) for way, where in enumerate(ways)
    ]
    relay = {}
    for step in range(CHUNKS):
        for way, where in enumerate(ways):
            part = relayed[way][step]
            relay[way, part] = block_to(1 + way, h_ref, where, chunks[part], part)
    near = [block_to(1 + way, h_ref, where, spans[1 - way], relayed[1 - way][0]) for way, where in enumerate(ways)]
    send_slots(0, outgoing, mine, d_send, d_recv, 1)

    far = []
    for step in range(CHUNKS):
        for way, where in enumerate(ways):
            part = relayed[way][step]
            relay[way, part].wait_recv()
            far.append(block_to(3, blocks.at[way], where, chunks[part], part))
        if step == 0:
            meta_near[0].wait_recv()
            far.append(go(remote(metas.at[0], metas.at[2], m_send.at[2], m_recv.at[2], up_ring)))
    meta_near[1].wait_recv()
    for way in range(2):
        near[way].wait_recv()
        place(1 + way)
        send_slots(1 + way, outgoing, mine, d_send, d_recv, 1)

    def exchange(group):
        for b in group:
            wait_slots(b, mine, d_recv)
        span = pl.ds(group[0], len(group))
        copy = remote(mine.at[span], other.at[span], x_send.at[group[0]], x_recv.at[group[0]], partner)
        return go(copy)

    def experts(group, swap):
        count = len(group) * rows
        span = pl.ds(group[0], len(group))
        swap.wait_recv()
        tokens_in = jnp.concatenate(
            [mine[span].reshape(count, width), other[span].reshape(count, width)], axis=1
        )
        step = 256
        for start in range(0, gate_w.shape[1], step):
            gate = jnp.dot(tokens_in, gate_w[:, start : start + step], preferred_element_type=jnp.float32)
            up = jnp.dot(tokens_in, up_w[:, start : start + step], preferred_element_type=jnp.float32)
            value = gate * (1.0 / (1.0 + jnp.exp(-gate))) * up
            act[pl.ds(0, count), start : start + step] = value.astype(jnp.bfloat16)
        active = act[pl.ds(0, count), :]
        away = jnp.dot(active, down_w[1], preferred_element_type=jnp.float32)
        part_out[span] = away.astype(jnp.bfloat16).reshape(len(group), rows, width)
        copy = go(remote(part_out.at[span], part_in.at[span], s_send.at[group[0]], s_recv.at[group[0]], partner))
        here = jnp.dot(active, down_w[0], preferred_element_type=jnp.float32)
        own_part[span] = here.astype(jnp.bfloat16).reshape(len(group), rows, width)
        return copy

    def answer(group, copy):
        copy.wait_recv()
        for b in group:
            both = own_part[b].astype(jnp.float32) + part_in[b].astype(jnp.float32)
            answers[b] = both.reshape(SLOTS, capacity, width).astype(jnp.bfloat16)
            send_slots(b, answers, returned, r_send, r_recv, -1)

    def combine(b):
        wait_slots(b, returned, r_recv)
        slots = returned[b].reshape(rows, width)
        return jnp.dot(weight_hi[b], slots, preferred_element_type=jnp.float32) + jnp.dot(
            weight_lo[b], slots, preferred_element_type=jnp.float32
        )

    for copy in far:
        copy.wait_recv()
    place(3)
    send_slots(3, outgoing, mine, d_send, d_recv, 1)

    for load in loads:
        load.wait()
    part_own = experts((0,), exchange((0,)))
    swap_near = [exchange((b,)) for b in (1, 2)]
    swap_far = exchange((3,))
    part_up = experts((1,), swap_near[0])
    part_far = experts((3,), swap_far)
    answer((0,), part_own)
    part_down = experts((2,), swap_near[1])
    answer((3,), part_far)
    answer((1,), part_up)
    answer((2,), part_down)

    travel[2] = combine(3).astype(jnp.bfloat16)
    back = (down_ring, up_ring)
    chains, finals = {}, []
    for step in range(CHUNKS):
        for way, where in enumerate(back):
            part = relayed[way][step]
            chains[way, part] = go(
                remote(travel.at[2, chunks[part]], chain_in.at[chunks[part]], c_send.at[part], c_recv.at[part], where)
            )
    for b in range(3):
        near_sum[b] = combine(b)

    def final_to(way, rows_in, sem):
        finals.append(
            go(
                remote(
                    travel.at[way, rows_in],
                    final_in.at[way, rows_in],
                    f_send.at[way, sem],
                    f_recv.at[way, sem],
                    back[way],
                )
            )
        )

    for way in range(2):
        rows_in = spans[1 - way]
        travel[way, rows_in] = near_sum[1 + way, rows_in].astype(jnp.bfloat16)
        final_to(way, rows_in, relayed[1 - way][0])
    for step in range(CHUNKS):
        for way in range(2):
            part = relayed[way][step]
            chains[way, part].wait_recv()
            total = near_sum[1 + way, chunks[part]] + chain_in[chunks[part]].astype(jnp.float32)
            travel[way, chunks[part]] = total.astype(jnp.bfloat16)
            final_to(way, chunks[part], part)
    for copy in finals:
        copy.wait_recv()
    combined = near_sum[0] + final_in[0].astype(jnp.float32) + final_in[1].astype(jnp.float32)
    squares = jnp.sum(combined * combined, axis=1, keepdims=True)
    square_out[...] = jnp.broadcast_to(squares, square_out.shape)
    copy = go(remote(square_out, square_in, q_send.at[0], q_recv.at[0], partner))
    copy.wait_recv()
    mean = (squares + square_in[:, :1]) / (2 * width)
    out_ref[...] = (combined * lax.rsqrt(mean + norm_eps) * gain_ref[...]).astype(jnp.bfloat16)

    for copy in first:
        copy.wait_send()
    for b in range(len(SOURCE)):
        wait_slots(b, outgoing, d_send)
        wait_slots(b, answers, r_send)


def solution(mesh):
    experts = mesh.shape["ep"]
    planes = experts // COLUMNS
    assert planes == STRIDE * len(SOURCE) and mesh.shape["tp"] == 2

    def shards(hidden_state, expert_ids, route_weight, gate_matrix, up_matrix, down_matrix, norm_gain):
        tokens, top = expert_ids.shape
        width = hidden_state.shape[1]
        hidden = gate_matrix.shape[2]
        capacity = max(2, 2 * tokens * top // experts)
        rows = SLOTS * capacity
        count = len(SOURCE)
        vmem, hbm = pl.BlockSpec(memory_space=pltpu.VMEM), pl.BlockSpec(memory_space=pltpu.HBM)
        slots = pltpu.VMEM((count, SLOTS, capacity, width), jnp.bfloat16)
        parts = pltpu.VMEM((count, rows, width), jnp.bfloat16)
        dma = pltpu.SemaphoreType.DMA
        return pl.pallas_call(
            functools.partial(kernel, planes),
            out_shape=pltpu.VMEM((tokens, width), jnp.bfloat16),
            in_specs=[hbm] * 7,
            out_specs=vmem,
            scratch_shapes=[
                pltpu.VMEM((tokens, width), jnp.bfloat16),
                pltpu.VMEM((top, tokens), jnp.int32),
                pltpu.VMEM((top, tokens), jnp.float32),
                pltpu.VMEM((1, width), jnp.float32),
                pltpu.VMEM((2 * top, LANES), jnp.float32),
                pltpu.VMEM((2 * width, hidden), jnp.bfloat16),
                pltpu.VMEM((2 * width, hidden), jnp.bfloat16),
                pltpu.VMEM((2, hidden, width), jnp.bfloat16),
                pltpu.VMEM((count - 1, tokens, width), jnp.bfloat16),
                pltpu.VMEM((count - 1, 2 * top, LANES), jnp.float32),
                slots,
                slots,
                slots,
                pltpu.VMEM((2 * rows, hidden), jnp.bfloat16),
                parts,
                parts,
                parts,
                slots,
                slots,
                pltpu.VMEM((count, tokens, rows), jnp.bfloat16),
                pltpu.VMEM((count, tokens, rows), jnp.bfloat16),
                pltpu.VMEM((3, tokens, width), jnp.float32),
                pltpu.VMEM((3, tokens, width), jnp.bfloat16),
                pltpu.VMEM((tokens, width), jnp.bfloat16),
                pltpu.VMEM((2, tokens, width), jnp.bfloat16),
                pltpu.VMEM((tokens, LANES), jnp.float32),
                pltpu.VMEM((tokens, LANES), jnp.float32),
                dma((4,)),
                dma((6,)),
                dma((3,)), dma((3,)),
                dma((3, 2 * CHUNKS)), dma((3, 2 * CHUNKS)),
                dma((count,)), dma((count,)),
                dma((count,)), dma((count,)),
                dma((count,)), dma((count,)),
                dma((count,)), dma((count,)),
                dma((2 * CHUNKS,)), dma((2 * CHUNKS,)),
                dma((2, 2 * CHUNKS)), dma((2, 2 * CHUNKS)),
                dma((1,)), dma((1,)),
            ],
            compiler_params=pltpu.CompilerParams(
                collective_id=0, has_side_effects=True, vmem_limit_bytes=64_000_000
            ),
        )(hidden_state, expert_ids.T, route_weight.T, norm_gain.reshape(1, width), gate_matrix, up_matrix, down_matrix)

    placed = (
        P(("grp", "ep"), "tp"),
        P(("grp", "ep"), None),
        P(("grp", "ep"), None),
        P("ep", None, "tp"),
        P("ep", None, "tp"),
        P("ep", "tp", None),
        P("tp"),
    )
    return jax.shard_map(
        shards, mesh=mesh, in_specs=placed, out_specs=P(("grp", "ep"), "tp"), check_vma=False
    )
```
